32 devices in a mesh: sp: 8 (over z, x), tp: 4 (over y, core).
Axes of the slice: x: 2, y: 2, z: 4, core: 2. Of those that a mesh axis runs over, the one named last changes fastest.
Arguments:
- queries: bfloat16 [8192, 1024], P('sp', 'tp'), may hold values from -6 to 6, as said below
- key_rows: bfloat16 [8192, 1024], P('sp', 'tp'), may hold values from -6 to 6, as said below
- value_rows: bfloat16 [8192, 1024], P('sp', 'tp'), may hold values from -6 to 6
- lambdas: float32 [8], P('tp'), may hold values from 0.3 to 0.8
- head_gain: float32 [128], replicated, may hold values from 0.1 to 1.9
- out_weight: bfloat16 [1024, 2048], replicated, may hold values from -0.1875 to 0.1875
- stream: bfloat16 [8192, 2048], P(('sp', 'tp')), may hold values from -6 to 6
- ffn_gain: float32 [2048], replicated, may hold values from 0.1 to 1.9
- routes: int32 [8192, 2], P(('sp', 'tp')), may hold values from 0 to 7, all different within a row; in each aligned block of 256 rows (0 to 255, 256 to 511, ...) at most 80 rows name the same one
- route_weight: float32 [8192, 2], P(('sp', 'tp')), may hold values from 0.1 to 1
- gate_weight: bfloat16 [8, 2048, 5120], P('sp', None, 'tp'), may hold values from -0.125 to 0.125
- up_weight: bfloat16 [8, 2048, 5120], P('sp', None, 'tp'), may hold values from -0.125 to 0.125
- down_weight: bfloat16 [8, 5120, 2048], P('sp', 'tp'), may hold values from -0.078125 to 0.078125
Outputs:
- layer_out: bfloat16 [8192, 2048], P(('sp', 'tp'))
The draws below stay inside these ranges and needn't reach their ends.
Inputs may be any that keep to these rules, and one draw needn't show every extreme that they name: Custom draw; the queries of a position meet only keys of the same or earlier positions. `key_rows`: custom draw. `routes`: each row names 2 different experts. In the 256 rows of one device no expert is named by more than 80 rows, and every draw reaches 80 on some device.
All inputs are finite; a program needn't handle non-finite values.
Results may differ from the reference program's by a relative error of at most 0.01.
Values may be sent and summed in bfloat16 or wider, within the bound.
A program may use at most 128 MiB of HBM per device.

```python
import math
import jax
import jax.numpy as jnp
import numpy as np
from jax import lax

D = 2048
HEADS = 8
DH = 64
FE = 5120
TOPK = 2
TOKENS = 8192
TOK_POST = 256
EXPERTS = 8
SLOTS = 80
N_TP = 4


def draw_pair(key):
    width = HEADS * 2 * DH
    base_query = jax.random.fold_in(key, 101)
    base_key = jax.random.fold_in(key, 202)
    query_part = jnp.clip(1.3 * jax.random.normal(base_query, (TOKENS, width), jnp.float32), -6.0, 6.0)
    key_part = jnp.clip(1.3 * jax.random.normal(base_key, (TOKENS, width), jnp.float32), -6.0, 6.0)
    return (query_part, key_part)


def draw_queries(key, part):
    return draw_pair(key)[0].astype(jnp.bfloat16)


def draw_key_rows(key, part):
    return draw_pair(key)[1].astype(jnp.bfloat16)


def block_levels(stream_key, dims, split, least, high):
    def one(axis_at, blocks):
        draws = jax.random.uniform(jax.random.fold_in(jax.random.fold_in(stream_key, 6), axis_at), (blocks,), jnp.float32, least / len(split), high / len(split))
        return jnp.repeat(jnp.exp(draws), dims[axis_at] // blocks).reshape((-1,) + (1,) * (len(dims) - axis_at - 1))

    loudness = one(*split[0])
    for cut in split[1:]:
        loudness = loudness * one(*cut)
    return loudness


def deal_out(own_key, own, number, rows, number_of, top, bound, slope):
    sequence = jax.random.permutation(own_key, number_of)
    packed, ordinary = load_shares(number_of, rows * top, bound, slope, True), load_shares(number_of, rows * top, bound, slope, False)
    places = jnp.arange(number_of)

    def named(tallies, offset_by):
        used = int((tallies > 0).sum())
        fixed = max(1, used // 4)
        passed = fixed + (places - fixed + offset_by * (used - fixed)) % max(1, number_of - fixed)
        return jnp.zeros((number_of,), jnp.int32).at[sequence[jnp.where(places < fixed, places, passed)]].set(jnp.asarray(tallies, jnp.int32))

    tallies = jnp.where(number % 4 == 0, named(packed, number // 4), named(ordinary, number - number // 4 - 1))
    mixed = jax.random.permutation(jax.random.fold_in(own, 3), number_of)
    donor, taker = mixed[0:number_of // 2 * 2:2], mixed[1:number_of // 2 * 2:2]
    margin = jnp.minimum(tallies[donor] - 1, bound - tallies[taker]) // 2
    margin = jnp.where((donor == sequence[0]) | (taker == sequence[0]) | (tallies[taker] == 0), 0, jnp.maximum(margin, 0))
    passed = jax.random.randint(jax.random.fold_in(own, 4), (number_of // 2,), 0, 1 << 20) % (margin + 1)
    tallies = tallies.at[donor].add(-passed).at[taker].add(passed)
    members = jnp.searchsorted(jnp.cumsum(tallies), jnp.arange(rows * top), side="right").astype(jnp.int32)
    listing = members.reshape(top, rows).T
    listing = listing[jax.random.permutation(jax.random.fold_in(own, 1), rows)]
    offset_by = jax.random.randint(jax.random.fold_in(own, 2), (rows, 1), 0, top)
    return jnp.take_along_axis(listing, (jnp.arange(top)[None, :] + offset_by) % top, axis=1)


def load_shares(amount, total, bound, lean, full):
    portions = [(1 << 20) // math.isqrt(grade ** lean) + 1 for grade in range(1, amount + 1)]
    largest = bound if full else min(bound, max(-(-total // amount), total * portions[0] // sum(portions)))
    least = 1 if total - largest >= amount - 1 else 0
    counts, surplus = [largest] + [least] * (amount - 1), total - largest - least * (amount - 1)
    while surplus > 0:
        free = [i for i in range(1, amount) if counts[i] < largest] or [i for i in range(1, amount) if counts[i] < bound]
        pool, budget = sum([portions[i] for i in free]), surplus
        for i in free:
            addition = min(bound - counts[i], max(1, budget * portions[i] // pool), surplus)
            counts[i] = counts[i] + addition
            surplus = surplus - addition
    return np.array(counts)


def normal_values(rng, dims, scale, limit, pieces=(), kind=jnp.bfloat16):
    entries = jax.random.normal(rng, dims, jnp.float32) * scale
    if len(pieces) > 0:
        entries = block_levels(rng, dims, pieces, -0.22, 0.18) * entries
    return jnp.clip(entries, min=-limit, max=limit).astype(kind)


def setup_inputs(seed: int = 0) -> dict:
    streams_of = jax.random.split(jax.random.key(seed), 14)
    queries = draw_queries(jax.random.fold_in(streams_of[13], 71), 0)
    key_rows = draw_key_rows(jax.random.fold_in(streams_of[13], 71), 0)
    value_rows = normal_values(streams_of[2], (TOKENS, HEADS * 2 * DH), 1.0, 6.0, ((0, 8), (1, 4)))
    lambdas = jnp.clip(0.3 + 0.5 * jax.random.uniform(streams_of[3], (HEADS,), jnp.float32) ** block_levels(streams_of[3], (HEADS,), ((0, 4),), -0.2, 0.2), 0.3, 0.8)
    head_gain = jnp.clip(1.0 + 0.18 * jax.random.normal(streams_of[4], (2 * DH,), jnp.float32), 0.1, 1.9)
    out_weight = normal_values(streams_of[5], (HEADS * 2 * DH, D), (HEADS * 2 * DH) ** -0.5, 0.1875)
    stream = normal_values(streams_of[6], (TOKENS, D), 1.0, 6.0, ((0, 32),))
    ffn_gain = jnp.clip(1.0 + 0.18 * jax.random.normal(streams_of[7], (D,), jnp.float32), 0.1, 1.9)
    routes_keys = jax.random.split(jax.random.fold_in(streams_of[8], 1), TOKENS // TOK_POST)
    routes_turns = jax.random.permutation(jax.random.fold_in(streams_of[8], 3), TOKENS // TOK_POST)
    routes = jax.vmap(lambda own, number: deal_out(jax.random.fold_in(streams_of[8], 2), own, number, TOK_POST, EXPERTS, TOPK, SLOTS, 1))(routes_keys, routes_turns).reshape((TOKENS, TOPK))
    route_weight = jnp.clip(0.1 + 0.9 * jax.random.uniform(streams_of[9], (TOKENS, TOPK), jnp.float32) ** block_levels(streams_of[9], (TOKENS, TOPK), ((0, 32),), -0.2, 0.2), 0.1, 1.0)
    gate_weight = normal_values(streams_of[10], (EXPERTS, D, FE), D ** -0.5, 0.125, ((0, 8), (2, 4)))
    up_weight = normal_values(streams_of[11], (EXPERTS, D, FE), D ** -0.5, 0.125, ((0, 8), (2, 4)))
    down_weight = normal_values(streams_of[12], (EXPERTS, FE, D), FE ** -0.5, 0.078125, ((0, 8), (1, 4)))
    return dict(queries=queries, key_rows=key_rows, value_rows=value_rows, lambdas=lambdas, head_gain=head_gain, out_weight=out_weight, stream=stream, ffn_gain=ffn_gain, routes=routes, route_weight=route_weight, gate_weight=gate_weight, up_weight=up_weight, down_weight=down_weight)


def attention(queries, key_rows, value_rows, lambdas, head_gain):
    tokens = queries.shape[0]
    q_all = queries.astype(jnp.float32).reshape(tokens, HEADS, 2, DH)
    k_all = key_rows.astype(jnp.float32).reshape(tokens, HEADS, 2, DH)
    v_all = value_rows.astype(jnp.float32).reshape(tokens, HEADS, 2 * DH)
    block = math.gcd(tokens, 256)
    key_pos = jnp.arange(tokens, dtype=jnp.int32)

    def attend(start):
        q_block = lax.dynamic_slice_in_dim(q_all, start, block, 0)
        scores = jnp.einsum('qhmd,khmd->hmqk', q_block, k_all) * DH ** (-0.5)
        query_pos = start + jnp.arange(block, dtype=jnp.int32)
        mask = key_pos[None, :] <= query_pos[:, None]
        scores = jnp.where(mask, scores, -jnp.inf)
        top = lax.optimization_barrier(jnp.max(scores, axis=-1, keepdims=True))
        expo = jnp.exp(scores - top)
        total = lax.optimization_barrier(jnp.sum(expo, axis=-1))
        weights = lax.optimization_barrier(expo.astype(jnp.bfloat16)).astype(jnp.float32)
        mixed = jnp.einsum('hmqk,khe->hmqe', weights, v_all) / total[..., None]
        contrast = mixed[:, 0] - lambdas[:, None, None] * mixed[:, 1]
        contrast = contrast * lax.rsqrt(lax.optimization_barrier(jnp.mean(contrast * contrast, axis=-1, keepdims=True)) + 1e-05) * head_gain
        return jnp.transpose(contrast, (1, 0, 2)).reshape(block, HEADS * 2 * DH).astype(jnp.bfloat16)
    starts = jnp.arange(tokens // block, dtype=jnp.int32) * block
    return lax.map(attend, starts).reshape(tokens, HEADS * 2 * DH)

def reference(queries, key_rows, value_rows, lambdas, head_gain, out_weight, stream, ffn_gain, routes, route_weight, gate_weight, up_weight, down_weight):
    tokens = queries.shape[0]
    heads_out = attention(queries, key_rows, value_rows, lambdas, head_gain)
    attended = stream.astype(jnp.float32) + jnp.dot(heads_out, out_weight, preferred_element_type=jnp.float32)
    normed = (attended * lax.rsqrt(lax.optimization_barrier(jnp.mean(attended * attended, axis=-1, keepdims=True)) + 1e-06) * ffn_gain).astype(jnp.bfloat16)
    capacity = tokens // TOK_POST * SLOTS

    def expert(carry, index):
        hits = routes == index
        weight = lax.optimization_barrier(jnp.sum(jnp.where(hits, route_weight, 0.0), axis=1))
        chosen = jnp.any(hits, axis=1)
        count = jnp.sum(chosen.astype(jnp.int32))
        picked = jnp.nonzero(chosen, size=capacity, fill_value=0)[0].astype(jnp.int32)
        rows = normed[picked]
        gate = jnp.dot(rows, gate_weight[index], preferred_element_type=jnp.float32)
        upper = jnp.dot(rows, up_weight[index], preferred_element_type=jnp.float32)
        act = (jax.nn.silu(gate) * upper).astype(jnp.bfloat16)
        parts = jnp.einsum('rcf,cfd->rcd', act.astype(jnp.float32).reshape(capacity, N_TP, FE // N_TP), down_weight[index].astype(jnp.float32).reshape(N_TP, FE // N_TP, D))
        parts = lax.optimization_barrier(parts.astype(jnp.bfloat16)).astype(jnp.float32)
        summed = lax.optimization_barrier(lax.optimization_barrier(jnp.sum(parts, axis=1)).astype(jnp.bfloat16)).astype(jnp.float32)
        valid = jnp.arange(capacity, dtype=jnp.int32) < count
        scale = jnp.where(valid, weight[picked], 0.0)
        return (carry.at[picked].add(summed * scale[:, None]), None)
    start = jnp.zeros((tokens, D), jnp.float32)
    routed, _ = lax.scan(expert, start, jnp.arange(EXPERTS, dtype=jnp.int32))
    return (attended + routed).astype(jnp.bfloat16)
```

```python
import functools
import math

import jax
import jax.numpy as jnp
from jax import lax
from jax.experimental import pallas as pl
from jax.experimental.pallas import tpu as pltpu
from jax.sharding import PartitionSpec as P

DH = 64


def moe_kernel(
    n,
    lanes,
    slots,
    out_ref,
    gate_hbm,
    up_hbm,
    down_hbm,
    back_ref,
    gate,
    up,
    down,
    rows,
    act,
    part,
    from_core,
    chip_sum,
    from_y,
    final,
    weight_sem,
    local_sem,
    a_send,
    a_recv,
    y_send,
    y_recv,
    c_send,
    c_recv,
    p_send,
    p_recv,
    q_send,
    q_recv,
    r_send,
    r_recv,
):
    sp = lax.axis_index("sp")
    tp = lax.axis_index("tp")
    core = tp % 2
    ypos = tp // 2
    other = ypos * 2 + (1 - core)
    half = lanes * slots

    def y_up(j):
        return ((ypos + j) % lanes) * 2 + core

    def y_down(j):
        return ((ypos + lanes - j) % lanes) * 2 + core

    def block(k, lane, j):
        return rows.at[k, pl.ds((lane * lanes + j) * slots, slots)]

    def remote(src, dst, send, recv, where):
        return pltpu.make_async_remote_copy(
            src_ref=src,
            dst_ref=dst,
            send_sem=send,
            recv_sem=recv,
            device_id=where,
            device_id_type=pl.DeviceIdType.MESH,
        )

    def exchange(k):
        goal = (sp + k) % n
        return remote(out_ref.at[goal], block(k, 0, 0), a_send.at[k], a_recv.at[k], (goal, tp))

    def across(k, j):
        return remote(
            block(k, 0, 0), block(k, 0, j), y_send.at[k, j], y_recv.at[k, j], (sp, y_up(j))
        )

    def relay(k, j):
        return remote(
            block(k, 0, j), block(k, 1, j), c_send.at[k, j], c_recv.at[k, j], (sp, other)
        )

    def core_part(k):
        return remote(
            part.at[k % 2, pl.ds(half, half)], from_core.at[k], p_send.at[k], p_recv.at[k], (sp, other)
        )

    def y_part(k, j):
        return remote(
            chip_sum.at[k, pl.ds(j * slots, slots)],
            from_y.at[k, pl.ds((j - 1) * slots, slots)],
            q_send.at[k, j],
            q_recv.at[k, j],
            (sp, y_down(j)),
        )

    def give_back(k):
        goal = (sp + n - k) % n
        return remote(final.at[k], back_ref.at[sp], r_send.at[k], r_recv.at[k], (goal, tp))

    weights = [
        pltpu.make_async_copy(a, b, weight_sem.at[i])
        for i, (a, b) in enumerate(((gate_hbm, gate), (up_hbm, up), (down_hbm, down)))
    ]
    for copy in weights:
        copy.start()
    own = pltpu.make_async_copy(out_ref.at[sp], block(0, 0, 0), local_sem.at[0])
    own.start()

    barrier = pltpu.get_barrier_semaphore()
    for k in range(1, n):
        pl.semaphore_signal(
            barrier, inc=1, device_id=((sp + k) % n, tp), device_id_type=pl.DeviceIdType.MESH
        )
    for k in range(1, 2 * lanes):
        pl.semaphore_signal(
            barrier,
            inc=1,
            device_id=(sp, (tp + k) % (2 * lanes)),
            device_id_type=pl.DeviceIdType.MESH,
        )
    pl.semaphore_wait(barrier, n + 2 * lanes - 2)

    @pl.loop(1, n)
    def _(k):
        exchange(k).start()

    def forward(k):
        for j in range(1, lanes):
            across(k, j).start()
        relay(k, 0).start()

    own.wait()
    forward(0)

    tile = math.gcd(gate.shape[1], 256)
    wide = math.gcd(down.shape[1], 256)

    @pl.loop(0, n + 3)
    def _(i):
        @pl.when(i < n - 1)
        def _():
            exchange(i + 1).wait_recv()
            forward(i + 1)

        @pl.when(i < n)
        def _():
            for j in range(1, lanes):
                across(i, j).wait_recv()
                relay(i, j).start()

        @pl.when((i >= 1) & (i < n + 1))
        def _():
            k = i - 1

            @pl.when(k == 0)
            def _():
                for copy in weights:
                    copy.wait()

            for j in range(lanes):
                relay(k, j).wait_recv()

            @pl.when(k >= 2)
            def _():
                core_part(k - 2).wait_send()

            @pl.loop(0, gate.shape[1] // tile)
            def _(f):
                cols = pl.ds(pl.multiple_of(f * tile, tile), tile)
                x = rows[k]
                g = jnp.dot(x, gate[:, cols], preferred_element_type=jnp.float32)
                u = jnp.dot(x, up[:, cols], preferred_element_type=jnp.float32)
                act[:, cols] = (g / (1.0 + jnp.exp(-g)) * u).astype(jnp.bfloat16)

            @pl.loop(0, down.shape[1] // wide)
            def _(d):
                cols = pl.ds(pl.multiple_of(d * wide, wide), wide)
                part[k % 2, :, cols] = jnp.dot(
                    act[...], down[:, cols], preferred_element_type=jnp.float32
                ).astype(jnp.bfloat16)

            core_part(k).start()

        @pl.when((i >= 2) & (i < n + 2))
        def _():
            k = i - 2
            core_part(k).wait_recv()

            @pl.loop(0, half // 16)
            def _(r):
                at = pl.ds(pl.multiple_of(r * 16, 16), 16)
                total = part[k % 2, at].astype(jnp.float32) + from_core[k, at].astype(jnp.float32)
                chip_sum[k, at] = total.astype(jnp.bfloat16)

            for j in range(1, lanes):
                y_part(k, j).start()

        @pl.when(i >= 3)
        def _():
            k = i - 3
            for j in range(1, lanes):
                y_part(k, j).wait_recv()

            @pl.loop(0, slots // 16)
            def _(r):
                at = pl.ds(pl.multiple_of(r * 16, 16), 16)
                total = chip_sum[k, at].astype(jnp.float32)
                for j in range(1, lanes):
                    here = pl.ds(pl.multiple_of((j - 1) * slots + r * 16, 16), 16)
                    total = total + from_y[k, here].astype(jnp.float32)
                final[k, at] = total.astype(jnp.bfloat16)

            @pl.when(k > 0)
            def _():
                give_back(k).start()

            @pl.when(k == 0)
            def _():
                pltpu.make_async_copy(final.at[0], back_ref.at[sp], local_sem.at[1]).start()

    pltpu.make_async_copy(final.at[0], back_ref.at[sp], local_sem.at[1]).wait()
    for k in (n - 2, n - 1):
        core_part(k).wait_send()

    @pl.loop(0, n)
    def _(k):
        @pl.when(k > 0)
        def _():
            exchange(k).wait_send()
            give_back(k).wait_send()
            give_back(k).wait_recv()

        for j in range(1, lanes):
            across(k, j).wait_send()
            y_part(k, j).wait_send()
        for j in range(lanes):
            relay(k, j).wait_send()


def exchange_and_apply(outgoing, gate_local, up_local, down_local):
    n, slots, width = outgoing.shape
    lanes = lax.axis_size("tp") // 2
    hidden = gate_local.shape[1]
    kind = jnp.bfloat16
    dma = pltpu.SemaphoreType.DMA
    flops = 6 * n * lanes * 2 * slots * width * hidden
    return pl.pallas_call(
        functools.partial(moe_kernel, n, lanes, slots),
        out_shape=jax.ShapeDtypeStruct((n, slots, width), kind),
        in_specs=[pl.BlockSpec(memory_space=pltpu.VMEM)]
        + [pl.BlockSpec(memory_space=pl.ANY)] * 3,
        out_specs=pl.BlockSpec(memory_space=pltpu.VMEM),
        scratch_shapes=[
            pltpu.VMEM((width, hidden), kind),
            pltpu.VMEM((width, hidden), kind),
            pltpu.VMEM((hidden, width), kind),
            pltpu.VMEM((n, 2 * lanes * slots, width), kind),
            pltpu.VMEM((2 * lanes * slots, hidden), kind),
            pltpu.VMEM((2, 2 * lanes * slots, width), kind),
            pltpu.VMEM((n, lanes * slots, width), kind),
            pltpu.VMEM((n, lanes * slots, width), kind),
            pltpu.VMEM((n, max(1, lanes - 1) * slots, width), kind),
            pltpu.VMEM((n, slots, width), kind),
            dma((3,)),
            dma((2,)),
            dma((n,)),
            dma((n,)),
            dma((n, lanes)),
            dma((n, lanes)),
            dma((n, lanes)),
            dma((n, lanes)),
            dma((n,)),
            dma((n,)),
            dma((n, lanes)),
            dma((n, lanes)),
            dma((n,)),
            dma((n,)),
        ],
        compiler_params=pltpu.CompilerParams(
            collective_id=0, has_side_effects=True, vmem_limit_bytes=67000000
        ),
        cost_estimate=pl.CostEstimate(
            flops=flops, bytes_accessed=6 * width * hidden, transcendentals=0
        ),
    )(outgoing, gate_local, up_local, down_local)


def attention_kernel(
    n,
    group,
    heads,
    post,
    q_ref,
    k_ref,
    v_ref,
    lam_ref,
    gain_ref,
    o_ref,
    keys,
    values,
    turned,
    asked,
    masked_q,
    maxima,
    accum,
    done,
    lam,
    kv_send,
    k_recv,
    v_recv,
    side_send,
    core_send,
    q_send,
    q_recv,
    lam_send,
    lam_recv,
    o_send,
    o_recv,
):
    sp = lax.axis_index("sp")
    tp = lax.axis_index("tp")
    tp_size = lax.axis_size("tp")
    core = tp % 2
    plane = tp // 2
    other = plane * 2 + (1 - core)
    in_plane = 2 * heads
    head = sp // group
    seat = sp % group
    source_core = head // heads
    is_source = core == source_core
    length = q_ref.shape[0]
    wide = 2 * DH
    chunks = 4 * group
    per_block = chunks // n
    size = length // per_block
    place = seat * 2 + core
    chunk_of = (place, chunks - 1 - place)
    parts = size // post

    def remote(src, dst, send, recv, where):
        return pltpu.make_async_remote_copy(
            src_ref=src,
            dst_ref=dst,
            send_sem=send,
            recv_sem=recv,
            device_id=where,
            device_id_type=pl.DeviceIdType.MESH,
        )

    barrier = pltpu.get_barrier_semaphore()
    everyone = n * tp_size
    me = sp * tp_size + tp

    @pl.loop(1, everyone)
    def _(k):
        to = (me + k) % everyone
        pl.semaphore_signal(
            barrier,
            inc=1,
            device_id=(to // tp_size, to % tp_size),
            device_id_type=pl.DeviceIdType.MESH,
        )

    pl.semaphore_wait(barrier, everyone - 1)

    def columns(h):
        return pl.ds(pl.multiple_of(h * wide, wide), wide)

    def turn_of(k):
        return jnp.where(head % 2 == 1, heads - 1 - k, k)

    def q_piece(k, i):
        h = turn_of(k)
        chunk = sp * per_block + i
        late = chunk >= 2 * group
        spot = jnp.where(late, chunks - 1 - chunk, chunk)
        slot = jnp.where(late, 1, 0)
        goal = (core * heads + h) * group + spot // 2
        goal_core = spot % 2
        src = q_ref.at[pl.ds(i * size, size), columns(h)]
        here = (goal == sp) & (goal_core == core)
        sem = q_send.at[k * per_block + i]
        far = remote(
            src, asked.at[slot], sem, q_recv.at[slot], (goal, plane * 2 + goal_core)
        )
        near = pltpu.make_async_copy(src, asked.at[slot], q_recv.at[slot])
        return here, far, near

    def kv_piece(k, which):
        h = turn_of(k)
        goal_head = core * heads + h
        here = goal_head == head
        src = k_ref.at[:, columns(h)] if which == 0 else turned.at[h]
        dst = (keys if which == 0 else values).at[sp]
        recv = (k_recv if which == 0 else v_recv).at[sp]
        far = remote(
            src, dst, kv_send.at[k * 2 + which], recv, (goal_head * group + seat, tp)
        )
        near = pltpu.make_async_copy(src, dst, recv)
        return here, far, near

    def launch(here, far, near):
        @pl.when(here)
        def _():
            near.start()

        @pl.when(jnp.logical_not(here))
        def _():
            far.start()

    pieces = [q_piece(k, i) for k in range(heads) for i in range(per_block)]
    pieces.append(kv_piece(0, 0))
    for piece in pieces:
        launch(*piece)
    for h in range(heads):
        block = v_ref[:, h * wide : (h + 1) * wide].astype(jnp.float32)
        turned[h] = jnp.transpose(block).astype(jnp.bfloat16)
    later = [kv_piece(0, 1)] + [kv_piece(k, which) for k in range(1, heads) for which in range(2)]
    for piece in later:
        launch(*piece)
    pieces += later
    for row in range(4):
        accum[row] = jnp.zeros(accum.shape[1:], jnp.float32)
        maxima[row] = jnp.full(maxima.shape[1:], -1e30, jnp.float32)

    def lam_copy():
        return remote(
            lam_ref.at[head % heads], lam, lam_send.at[0], lam_recv.at[0], (sp, other)
        )

    @pl.when(is_source)
    def _():
        lam_copy().start()

    lane = lax.broadcasted_iota(jnp.int32, (wide, size), 0)
    for slot in range(2):
        pltpu.make_async_copy(asked.at[slot], asked.at[slot], q_recv.at[slot]).wait()
        turn = jnp.transpose(asked[slot].astype(jnp.float32)) * (DH ** (-0.5) * math.log2(math.e))
        high = turn.astype(jnp.bfloat16)
        low = (turn - high.astype(jnp.float32)).astype(jnp.bfloat16)
        for m in range(2):
            keep = (lane >= m * DH) & (lane < (m + 1) * DH)
            masked_q[slot * 2 + m, 0:wide] = jnp.where(keep, high, jnp.zeros_like(high))
            masked_q[slot * 2 + m, wide : 2 * wide] = jnp.where(keep, low, jnp.zeros_like(low))

    def source_of(w):
        t = w // group
        r = w % group
        b = (head % 2 + t % 2) % 2 + 2 * ((head // 2 + t // 2) % 2)
        return b * group + (seat + r) % group, r

    def sideways(s, r, which):
        buf = (keys if which == 0 else values).at[s]
        recv = (k_recv if which == 0 else v_recv).at[s]
        goal = head * group + (seat + r) % group
        return remote(buf, buf, side_send.at[s, r, which], recv, (goal, tp))

    def to_core(s, which):
        buf = (keys if which == 0 else values).at[s]
        recv = (k_recv if which == 0 else v_recv).at[s]
        return remote(buf, buf, core_send.at[s, which], recv, (sp, other))

    def receive(w):
        s, r = source_of(w)
        for which in range(2):
            to_core(s, which).wait_recv()

            @pl.when(is_source)
            def _(which=which):
                @pl.when(r == 0)
                def _():
                    for k in range(1, group):
                        sideways(s, k, which).start()

                to_core(s, which).start()

    tall = math.gcd(length, 512)

    def attend(slot, s, chunk, diagonal):
        for first in range(0, length, tall):
            k = keys[s, first : first + tall]
            k = jnp.concatenate([k, k], axis=1)
            v = values[s, :, first : first + tall]
            v = jnp.concatenate([v, jnp.ones((16, tall), jnp.bfloat16)], axis=0)
            for m in range(2):
                row = slot * 2 + m
                scores = jnp.dot(k, masked_q[row], preferred_element_type=jnp.float32)
                if diagonal:
                    k_pos = s * length + first + lax.broadcasted_iota(jnp.int32, scores.shape, 0)
                    q_pos = chunk * size + lax.broadcasted_iota(jnp.int32, scores.shape, 1)
                    scores = jnp.where(k_pos <= q_pos, scores, -1e30)
                old = maxima[row, 0:1]
                top = jnp.maximum(jnp.max(scores, axis=0, keepdims=True), old)
                weights = jnp.exp2(scores - top).astype(jnp.bfloat16)
                mixed = jnp.dot(v, weights, preferred_element_type=jnp.float32)
                accum[row] = accum[row] * jnp.exp2(old - top) + mixed
                maxima[row] = jnp.broadcast_to(top, maxima.shape[1:])

    def step(slot, w):
        s, _ = source_of(w)
        chunk = jnp.where(slot == 0, chunk_of[0], chunk_of[1])
        block = chunk // per_block

        @pl.when(s == block)
        def _():
            attend(slot, s, chunk, True)

        @pl.when(s < block)
        def _():
            attend(slot, s, chunk, False)

    receive(0)

    @pl.loop(0, n)
    def _(w):
        @pl.when(w + 1 < n)
        def _():
            receive(w + 1)

        @pl.when(w < n - group)
        def _():
            @pl.loop(0, 2)
            def _(slot):
                step(slot, w)

    @pl.when(is_source)
    def _():
        lam[...] = lam_ref[head % heads]

    @pl.when(jnp.logical_not(is_source))
    def _():
        lam_copy().wait_recv()

    full_head = plane * in_plane + head

    def hand_over(slot, i):
        chunk = chunk_of[slot]
        goal = chunk // per_block
        goal_tp = (chunk % per_block) * parts + i
        here = (goal == sp) & (goal_tp == tp)
        src = done.at[slot, pl.ds(i * post, post)]
        dst = o_ref.at[:, pl.ds(pl.multiple_of(full_head * wide, wide), wide)]
        far = remote(src, dst, o_send.at[slot * parts + i], o_recv.at[full_head], (goal, goal_tp))
        near = pltpu.make_async_copy(src, dst, o_recv.at[full_head])
        return here, far, near

    handed = [[hand_over(slot, i) for i in range(parts)] for slot in range(2)]

    @pl.loop(0, 2)
    def _(slot):
        @pl.loop(n - group, n)
        def _(w):
            step(slot, w)

        one = accum[slot * 2, 0:wide] * (1.0 / accum[slot * 2, wide : wide + 1])
        two = accum[slot * 2 + 1, 0:wide] * (1.0 / accum[slot * 2 + 1, wide : wide + 1])
        contrast = one - lam[0:1, 0:1] * two
        square = jnp.mean(contrast * contrast, axis=0, keepdims=True)
        contrast = jnp.transpose(contrast * lax.rsqrt(square + 1e-05)) * gain_ref[...]
        done[slot] = contrast.astype(jnp.bfloat16)
        for k in range(2):
            @pl.when(slot == k)
            def _(k=k):
                for piece in handed[k]:
                    launch(*piece)

    for h in range(in_plane * (tp_size // 2)):
        part = o_ref.at[:, pl.ds(h * wide, wide)]
        pltpu.make_async_copy(part, part, o_recv.at[h]).wait()

    for here, far, near in pieces + handed[0] + handed[1]:
        @pl.when(jnp.logical_not(here))
        def _(far=far):
            far.wait_send()

    @pl.when(is_source)
    def _():
        lam_copy().wait_send()

        @pl.loop(0, n)
        def _(w):
            s, r = source_of(w)
            for which in range(2):
                to_core(s, which).wait_send()

                @pl.when(r == 0)
                def _(which=which):
                    for k in range(1, group):
                        sideways(s, k, which).wait_send()


def attention(queries, key_rows, value_rows, lambdas, head_gain):
    n = lax.axis_size("sp")
    tp_size = lax.axis_size("tp")
    length, columns = queries.shape
    wide = 2 * DH
    heads = columns // wide
    group = n // (2 * heads)
    chunks = 4 * group
    size = length * n // chunks
    post = length // tp_size
    kind = jnp.bfloat16
    dma = pltpu.SemaphoreType.DMA
    vmem = pl.BlockSpec(memory_space=pltpu.VMEM)
    return pl.pallas_call(
        functools.partial(attention_kernel, n, group, heads, post),
        out_shape=jax.ShapeDtypeStruct((post, columns * tp_size), kind),
        in_specs=[vmem] * 5,
        out_specs=vmem,
        scratch_shapes=[
            pltpu.VMEM((n, length, wide), kind),
            pltpu.VMEM((n, wide, length), kind),
            pltpu.VMEM((heads, wide, length), kind),
            pltpu.VMEM((2, size, wide), kind),
            pltpu.VMEM((4, 2 * wide, size), kind),
            pltpu.VMEM((4, 8, size), jnp.float32),
            pltpu.VMEM((4, wide + 16, size), jnp.float32),
            pltpu.VMEM((2, size, wide), kind),
            pltpu.VMEM((8, wide), jnp.float32),
            dma((2 * heads,)),
            dma((n,)),
            dma((n,)),
            dma((n, group, 2)),
            dma((n, 2)),
            dma((heads * chunks // n,)),
            dma((2,)),
            dma((1,)),
            dma((1,)),
            dma((2 * (size // post),)),
            dma((heads * tp_size,)),
        ],
        compiler_params=pltpu.CompilerParams(
            collective_id=1, has_side_effects=True, vmem_limit_bytes=60000000
        ),
    )(
        queries,
        key_rows,
        value_rows,
        jnp.broadcast_to(lambdas[:, None, None], (heads, 8, wide)),
        head_gain[None, :],
    )


def local(
    queries,
    key_rows,
    value_rows,
    lambdas,
    head_gain,
    out_weight,
    stream,
    ffn_gain,
    routes,
    route_weight,
    gate_weight,
    up_weight,
    down_weight,
):
    heads_local = attention(queries, key_rows, value_rows, lambdas, head_gain)
    attended = stream.astype(jnp.float32) + jnp.dot(
        heads_local, out_weight, preferred_element_type=jnp.float32
    )
    normed = (
        attended
        * lax.rsqrt(jnp.mean(attended * attended, axis=-1, keepdims=True) + 1e-06)
        * ffn_gain
    ).astype(jnp.bfloat16)
    rows_local = normed.shape[0]
    width = normed.shape[1]
    top_count = routes.shape[1]
    sp_size = lax.axis_size("sp")
    experts = sp_size * gate_weight.shape[0]
    slots = max(2, (rows_local * top_count * 5 + 4 * experts - 1) // (4 * experts))
    slots = -(-slots // 16) * 16
    flat_routes = routes.reshape(-1)
    onehot = (flat_routes[:, None] == jnp.arange(experts, dtype=jnp.int32)[None, :]).astype(
        jnp.int32
    )
    before = jnp.cumsum(onehot, axis=0) - onehot
    slot = jnp.sum(before * onehot, axis=1)
    target = flat_routes * slots + slot
    placed = (target[:, None] == jnp.arange(experts * slots, dtype=jnp.int32)[None, :]).astype(
        jnp.float32
    )
    placed = placed.reshape(rows_local, top_count, experts * slots)
    dispatch = jnp.transpose(jnp.sum(placed, axis=1)).astype(jnp.bfloat16)
    combine = jnp.einsum("tk,tks->ts", route_weight, placed, precision=lax.Precision.HIGHEST)
    outgoing = (
        jnp.dot(dispatch, normed, preferred_element_type=jnp.float32)
        .astype(jnp.bfloat16)
        .reshape(experts, slots, width)
    )
    gate_local = gate_weight[0]
    up_local = up_weight[0]
    down_local = down_weight[0]
    returned = exchange_and_apply(outgoing, gate_local, up_local, down_local).reshape(
        experts * slots, width
    )
    routed = jnp.dot(combine, returned.astype(jnp.float32), precision=lax.Precision.HIGHEST)
    return (attended + routed).astype(jnp.bfloat16)


def solution(mesh):
    placed = (
        P("sp", "tp"),
        P("sp", "tp"),
        P("sp", "tp"),
        P("tp"),
        P(),
        P(),
        P(("sp", "tp"), None),
        P(),
        P(("sp", "tp"), None),
        P(("sp", "tp"), None),
        P("sp", None, "tp"),
        P("sp", None, "tp"),
        P("sp", "tp", None),
    )
    return jax.shard_map(
        local, mesh=mesh, in_specs=placed, out_specs=P(("sp", "tp"), None), check_vma=False
    )
```

```python
import functools
import math

import jax
import jax.numpy as jnp
from jax import lax
from jax.experimental import pallas as pl
from jax.experimental.pallas import tpu as pltpu
from jax.sharding import PartitionSpec as P

DH = 64


def moe_kernel(
    n,
    lanes,
    slots,
    out_ref,
    gate_hbm,
    up_hbm,
    down_hbm,
    back_ref,
    gate,
    up,
    down,
    rows,
    act,
    part,
    from_core,
    chip_sum,
    from_y,
    final,
    weight_sem,
    local_sem,
    a_send,
    a_recv,
    y_send,
    y_recv,
    c_send,
    c_recv,
    p_send,
    p_recv,
    q_send,
    q_recv,
    r_send,
    r_recv,
):
    sp = lax.axis_index("sp")
    tp = lax.axis_index("tp")
    core = tp % 2
    ypos = tp // 2
    other = ypos * 2 + (1 - core)
    half = lanes * slots

    def y_up(j):
        return ((ypos + j) % lanes) * 2 + core

    def y_down(j):
        return ((ypos + lanes - j) % lanes) * 2 + core

    def block(k, lane, j):
        return rows.at[k, pl.ds((lane * lanes + j) * slots, slots)]

    def remote(src, dst, send, recv, where):
        return pltpu.make_async_remote_copy(
            src_ref=src,
            dst_ref=dst,
            send_sem=send,
            recv_sem=recv,
            device_id=where,
            device_id_type=pl.DeviceIdType.MESH,
        )

    near = n // 2

    def order(i):
        return i

    def partner(k):
        goal = 0
        bit = 1
        while bit < n:
            goal = goal + (sp // bit + k // bit) % 2 * bit
            bit *= 2
        return goal

    def exchange(k):
        goal = partner(k)
        return remote(out_ref.at[goal], block(k, 0, 0), a_send.at[k], a_recv.at[k], (goal, tp))

    def across(k, j):
        return remote(
            block(k, 0, 0), block(k, 0, j), y_send.at[k, j], y_recv.at[k, j], (sp, y_up(j))
        )

    def relay(k, j):
        return remote(
            block(k, 0, j), block(k, 1, j), c_send.at[k, j], c_recv.at[k, j], (sp, other)
        )

    def core_part(i):
        k = order(i)
        return remote(
            part.at[i % 2, pl.ds(half, half)], from_core.at[k], p_send.at[k], p_recv.at[k], (sp, other)
        )

    def y_part(k, j):
        return remote(
            chip_sum.at[k, pl.ds(j * slots, slots)],
            from_y.at[k, pl.ds((j - 1) * slots, slots)],
            q_send.at[k, j],
            q_recv.at[k, j],
            (sp, y_down(j)),
        )

    def give_back(k):
        goal = partner(k)
        return remote(final.at[k], back_ref.at[sp], r_send.at[k], r_recv.at[k], (goal, tp))

    weights = [
        pltpu.make_async_copy(a, b, weight_sem.at[i])
        for i, (a, b) in enumerate(((gate_hbm, gate), (up_hbm, up), (down_hbm, down)))
    ]
    for copy in weights:
        copy.start()
    own = pltpu.make_async_copy(out_ref.at[sp], block(0, 0, 0), local_sem.at[0])
    own.start()

    barrier = pltpu.get_barrier_semaphore()
    for k in range(1, n):
        pl.semaphore_signal(
            barrier, inc=1, device_id=((sp + k) % n, tp), device_id_type=pl.DeviceIdType.MESH
        )
    for k in range(1, 2 * lanes):
        pl.semaphore_signal(
            barrier,
            inc=1,
            device_id=(sp, (tp + k) % (2 * lanes)),
            device_id_type=pl.DeviceIdType.MESH,
        )
    pl.semaphore_wait(barrier, n + 2 * lanes - 2)

    @pl.loop(1, n)
    def _(k):
        exchange(k).start()

    def forward(k):
        for j in range(1, lanes):
            across(k, j).start()
        relay(k, 0).start()

    own.wait()
    forward(0)

    tile = math.gcd(gate.shape[1], 256)
    wide = math.gcd(down.shape[1], 256)

    def enter(i):
        k = order(i)
        exchange(k).wait_recv()
        forward(k)

    def spread(i):
        k = order(i)
        for j in range(1, lanes):
            across(k, j).wait_recv()
            relay(k, j).start()

    def compute(i):
        k = order(i)

        @pl.when(i == 0)
        def _():
            for copy in weights:
                copy.wait()

        for j in range(lanes):
            relay(k, j).wait_recv()

        @pl.when(i >= 2)
        def _():
            core_part(i - 2).wait_send()

        @pl.loop(0, gate.shape[1] // tile)
        def _(f):
            cols = pl.ds(pl.multiple_of(f * tile, tile), tile)
            x = rows[k]
            g = jnp.dot(x, gate[:, cols], preferred_element_type=jnp.float32)
            u = jnp.dot(x, up[:, cols], preferred_element_type=jnp.float32)
            act[:, cols] = (g / (1.0 + jnp.exp(-g)) * u).astype(jnp.bfloat16)

        @pl.loop(0, down.shape[1] // wide)
        def _(d):
            cols = pl.ds(pl.multiple_of(d * wide, wide), wide)
            part[i % 2, :, cols] = jnp.dot(
                act[...], down[:, cols], preferred_element_type=jnp.float32
            ).astype(jnp.bfloat16)

        core_part(i).start()

    def reduce(i):
        k = order(i)
        core_part(i).wait_recv()

        @pl.loop(0, half // 16)
        def _(r):
            at = pl.ds(pl.multiple_of(r * 16, 16), 16)
            total = part[i % 2, at].astype(jnp.float32) + from_core[k, at].astype(jnp.float32)
            chip_sum[k, at] = total.astype(jnp.bfloat16)

    def cross(i):
        for j in range(1, lanes):
            y_part(order(i), j).start()

    def finish(i):
        k = order(i)
        for j in range(1, lanes):
            y_part(k, j).wait_recv()

        @pl.loop(0, slots // 16)
        def _(r):
            at = pl.ds(pl.multiple_of(r * 16, 16), 16)
            total = chip_sum[k, at].astype(jnp.float32)
            for j in range(1, lanes):
                here = pl.ds(pl.multiple_of((j - 1) * slots + r * 16, 16), 16)
                total = total + from_y[k, here].astype(jnp.float32)
            final[k, at] = total.astype(jnp.bfloat16)

        @pl.when(k > 0)
        def _():
            give_back(k).start()

        @pl.when(k == 0)
        def _():
            pltpu.make_async_copy(final.at[0], back_ref.at[sp], local_sem.at[1]).start()

    def urgent(i):
        return (i == 0) | (i >= near)

    @pl.loop(0, n + 3)
    def _(i):
        @pl.when(i < n - 1)
        def _():
            enter(i + 1)

        @pl.when(i < n)
        def _():
            spread(i)

        @pl.when((i >= 1) & (i < n + 1))
        def _():
            compute(i - 1)

        @pl.when((i >= 2) & (i < n + 2))
        def _():
            reduce(i - 2)

            @pl.when(urgent(i - 2))
            def _():
                cross(i - 2)

        @pl.when(i == n + 1)
        def _():
            @pl.loop(1, near)
            def _(k):
                cross(k)

        @pl.when((i >= 3) & urgent(i - 3))
        def _():
            finish(i - 3)

    @pl.loop(1, near)
    def _(k):
        finish(k)

    pltpu.make_async_copy(final.at[0], back_ref.at[sp], local_sem.at[1]).wait()
    for i in (n - 2, n - 1):
        core_part(i).wait_send()

    @pl.loop(0, n)
    def _(k):
        @pl.when(k > 0)
        def _():
            exchange(k).wait_send()
            give_back(k).wait_send()
            give_back(k).wait_recv()

        for j in range(1, lanes):
            across(k, j).wait_send()
            y_part(k, j).wait_send()
        for j in range(lanes):
            relay(k, j).wait_send()


def exchange_and_apply(outgoing, gate_local, up_local, down_local):
    n, slots, width = outgoing.shape
    lanes = lax.axis_size("tp") // 2
    hidden = gate_local.shape[1]
    kind = jnp.bfloat16
    dma = pltpu.SemaphoreType.DMA
    flops = 6 * n * lanes * 2 * slots * width * hidden
    return pl.pallas_call(
        functools.partial(moe_kernel, n, lanes, slots),
        out_shape=jax.ShapeDtypeStruct((n, slots, width), kind),
        in_specs=[pl.BlockSpec(memory_space=pltpu.VMEM)]
        + [pl.BlockSpec(memory_space=pl.ANY)] * 3,
        out_specs=pl.BlockSpec(memory_space=pltpu.VMEM),
        scratch_shapes=[
            pltpu.VMEM((width, hidden), kind),
            pltpu.VMEM((width, hidden), kind),
            pltpu.VMEM((hidden, width), kind),
            pltpu.VMEM((n, 2 * lanes * slots, width), kind),
            pltpu.VMEM((2 * lanes * slots, hidden), kind),
            pltpu.VMEM((2, 2 * lanes * slots, width), kind),
            pltpu.VMEM((n, lanes * slots, width), kind),
            pltpu.VMEM((n, lanes * slots, width), kind),
            pltpu.VMEM((n, max(1, lanes - 1) * slots, width), kind),
            pltpu.VMEM((n, slots, width), kind),
            dma((3,)),
            dma((2,)),
            dma((n,)),
            dma((n,)),
            dma((n, lanes)),
            dma((n, lanes)),
            dma((n, lanes)),
            dma((n, lanes)),
            dma((n,)),
            dma((n,)),
            dma((n, lanes)),
            dma((n, lanes)),
            dma((n,)),
            dma((n,)),
        ],
        compiler_params=pltpu.CompilerParams(
            collective_id=0, has_side_effects=True, vmem_limit_bytes=67000000
        ),
        cost_estimate=pl.CostEstimate(
            flops=flops, bytes_accessed=6 * width * hidden, transcendentals=0
        ),
    )(outgoing, gate_local, up_local, down_local)


def attention_kernel(
    n,
    group,
    heads,
    post,
    q_ref,
    k_ref,
    v_ref,
    lam_ref,
    gain_ref,
    o_ref,
    keys,
    values,
    turned,
    asked,
    masked_q,
    maxima,
    accum,
    done,
    lam,
    kv_send,
    k_recv,
    v_recv,
    side_send,
    core_send,
    q_send,
    q_recv,
    lam_send,
    lam_recv,
    o_send,
    o_recv,
):
    sp = lax.axis_index("sp")
    tp = lax.axis_index("tp")
    tp_size = lax.axis_size("tp")
    core = tp % 2
    plane = tp // 2
    other = plane * 2 + (1 - core)
    in_plane = 2 * heads
    head = sp // group
    seat = sp % group
    source_core = head // heads
    is_source = core == source_core
    length = q_ref.shape[0]
    wide = 2 * DH
    chunks = 4 * group
    per_block = chunks // n
    size = length // per_block
    place = seat * 2 + core
    chunk_of = (place, chunks - 1 - place)
    parts = size // post

    def remote(src, dst, send, recv, where):
        return pltpu.make_async_remote_copy(
            src_ref=src,
            dst_ref=dst,
            send_sem=send,
            recv_sem=recv,
            device_id=where,
            device_id_type=pl.DeviceIdType.MESH,
        )

    barrier = pltpu.get_barrier_semaphore()
    everyone = n * tp_size
    me = sp * tp_size + tp

    @pl.loop(1, everyone)
    def _(k):
        to = (me + k) % everyone
        pl.semaphore_signal(
            barrier,
            inc=1,
            device_id=(to // tp_size, to % tp_size),
            device_id_type=pl.DeviceIdType.MESH,
        )

    pl.semaphore_wait(barrier, everyone - 1)

    def columns(h):
        return pl.ds(pl.multiple_of(h * wide, wide), wide)

    def turn_of(k):
        return jnp.where(head % 2 == 1, heads - 1 - k, k)

    def q_piece(k, i):
        h = turn_of(k)
        chunk = sp * per_block + i
        late = chunk >= 2 * group
        spot = jnp.where(late, chunks - 1 - chunk, chunk)
        slot = jnp.where(late, 1, 0)
        goal = (core * heads + h) * group + spot // 2
        goal_core = spot % 2
        src = q_ref.at[pl.ds(i * size, size), columns(h)]
        here = (goal == sp) & (goal_core == core)
        sem = q_send.at[k * per_block + i]
        far = remote(
            src, asked.at[slot], sem, q_recv.at[slot], (goal, plane * 2 + goal_core)
        )
        near = pltpu.make_async_copy(src, asked.at[slot], q_recv.at[slot])
        return here, far, near

    def kv_piece(k, which):
        h = turn_of(k)
        goal_head = core * heads + h
        here = goal_head == head
        src = k_ref.at[:, columns(h)] if which == 0 else turned.at[h]
        dst = (keys if which == 0 else values).at[sp]
        recv = (k_recv if which == 0 else v_recv).at[sp]
        far = remote(
            src, dst, kv_send.at[k * 2 + which], recv, (goal_head * group + seat, tp)
        )
        near = pltpu.make_async_copy(src, dst, recv)
        return here, far, near

    def launch(here, far, near):
        @pl.when(here)
        def _():
            near.start()

        @pl.when(jnp.logical_not(here))
        def _():
            far.start()

    pieces = [q_piece(k, i) for k in range(heads) for i in range(per_block)]
    pieces.append(kv_piece(0, 0))
    for piece in pieces:
        launch(*piece)
    for h in range(heads):
        block = v_ref[:, h * wide : (h + 1) * wide].astype(jnp.float32)
        turned[h] = jnp.transpose(block).astype(jnp.bfloat16)
    later = [kv_piece(0, 1)] + [kv_piece(k, which) for k in range(1, heads) for which in range(2)]
    for piece in later:
        launch(*piece)
    pieces += later
    for row in range(4):
        accum[row] = jnp.zeros(accum.shape[1:], jnp.float32)
        maxima[row] = jnp.full(maxima.shape[1:], -1e30, jnp.float32)

    def lam_copy():
        return remote(
            lam_ref.at[head % heads], lam, lam_send.at[0], lam_recv.at[0], (sp, other)
        )

    @pl.when(is_source)
    def _():
        lam_copy().start()

    lane = lax.broadcasted_iota(jnp.int32, (wide, size), 0)
    for slot in range(2):
        pltpu.make_async_copy(asked.at[slot], asked.at[slot], q_recv.at[slot]).wait()
        turn = jnp.transpose(asked[slot].astype(jnp.float32)) * (DH ** (-0.5) * math.log2(math.e))
        high = turn.astype(jnp.bfloat16)
        low = (turn - high.astype(jnp.float32)).astype(jnp.bfloat16)
        for m in range(2):
            keep = (lane >= m * DH) & (lane < (m + 1) * DH)
            masked_q[slot * 2 + m, 0:wide] = jnp.where(keep, high, jnp.zeros_like(high))
            masked_q[slot * 2 + m, wide : 2 * wide] = jnp.where(keep, low, jnp.zeros_like(low))

    def source_of(w):
        t = w // group
        r = w % group
        b = (head % 2 + t % 2) % 2 + 2 * ((head // 2 + t // 2) % 2)
        return b * group + (seat + r) % group, r

    def sideways(s, r, which):
        buf = (keys if which == 0 else values).at[s]
        recv = (k_recv if which == 0 else v_recv).at[s]
        goal = head * group + (seat + r) % group
        return remote(buf, buf, side_send.at[s, r, which], recv, (goal, tp))

    def to_core(s, which):
        buf = (keys if which == 0 else values).at[s]
        recv = (k_recv if which == 0 else v_recv).at[s]
        return remote(buf, buf, core_send.at[s, which], recv, (sp, other))

    def receive(w):
        s, r = source_of(w)
        for which in range(2):
            to_core(s, which).wait_recv()

            @pl.when(is_source)
            def _(which=which):
                @pl.when(r == 0)
                def _():
                    for k in range(1, group):
                        sideways(s, k, which).start()

                to_core(s, which).start()

    tall = math.gcd(length, 512)

    def attend(slot, s, chunk, diagonal):
        for first in range(0, length, tall):
            k = keys[s, first : first + tall]
            k = jnp.concatenate([k, k], axis=1)
            v = values[s, :, first : first + tall]
            v = jnp.concatenate([v, jnp.ones((16, tall), jnp.bfloat16)], axis=0)
            for m in range(2):
                row = slot * 2 + m
                scores = jnp.dot(k, masked_q[row], preferred_element_type=jnp.float32)
                if diagonal:
                    k_pos = s * length + first + lax.broadcasted_iota(jnp.int32, scores.shape, 0)
                    q_pos = chunk * size + lax.broadcasted_iota(jnp.int32, scores.shape, 1)
                    scores = jnp.where(k_pos <= q_pos, scores, -1e30)
                old = maxima[row, 0:1]
                top = jnp.maximum(jnp.max(scores, axis=0, keepdims=True), old)
                weights = jnp.exp2(scores - top).astype(jnp.bfloat16)
                mixed = jnp.dot(v, weights, preferred_element_type=jnp.float32)
                accum[row] = accum[row] * jnp.exp2(old - top) + mixed
                maxima[row] = jnp.broadcast_to(top, maxima.shape[1:])

    def step(slot, w):
        s, _ = source_of(w)
        chunk = jnp.where(slot == 0, chunk_of[0], chunk_of[1])
        block = chunk // per_block

        @pl.when(s == block)
        def _():
            attend(slot, s, chunk, True)

        @pl.when(s < block)
        def _():
            attend(slot, s, chunk, False)

    def slot_of(i):
        return jnp.where(2 * sp < n, 1 - i, i)

    rounds = n // group

    receive(0)

    @pl.loop(0, rounds)
    def _(t):
        @pl.loop(0, group)
        def _(r):
            @pl.when(r > 0)
            def _():
                receive(t * group + r)

            @pl.when((r == group - 1) & (t < rounds - 1))
            def _():
                receive((t + 1) * group)

            @pl.loop(0, jnp.where(t < rounds - 1, 2, 1))
            def _(i):
                step(slot_of(i), t * group + r)

    @pl.when(is_source)
    def _():
        lam[...] = lam_ref[head % heads]

    @pl.when(jnp.logical_not(is_source))
    def _():
        lam_copy().wait_recv()

    full_head = plane * in_plane + head

    def hand_over(slot, i):
        chunk = chunk_of[slot]
        goal = chunk // per_block
        goal_tp = (chunk % per_block) * parts + i
        here = (goal == sp) & (goal_tp == tp)
        src = done.at[slot, pl.ds(i * post, post)]
        dst = o_ref.at[:, pl.ds(pl.multiple_of(full_head * wide, wide), wide)]
        far = remote(src, dst, o_send.at[slot * parts + i], o_recv.at[full_head], (goal, goal_tp))
        near = pltpu.make_async_copy(src, dst, o_recv.at[full_head])
        return here, far, near

    handed = [[hand_over(slot, i) for i in range(parts)] for slot in range(2)]

    @pl.loop(0, 2)
    def _(i):
        slot = slot_of(i)

        @pl.when(i == 1)
        def _():
            @pl.loop(n - group, n)
            def _(w):
                step(slot, w)

        one = accum[slot * 2, 0:wide] * (1.0 / accum[slot * 2, wide : wide + 1])
        two = accum[slot * 2 + 1, 0:wide] * (1.0 / accum[slot * 2 + 1, wide : wide + 1])
        contrast = one - lam[0:1, 0:1] * two
        square = jnp.mean(contrast * contrast, axis=0, keepdims=True)
        contrast = jnp.transpose(contrast * lax.rsqrt(square + 1e-05)) * gain_ref[...]
        done[slot] = contrast.astype(jnp.bfloat16)
        for k in range(2):
            @pl.when(slot == k)
            def _(k=k):
                for piece in handed[k]:
                    launch(*piece)

    for h in range(in_plane * (tp_size // 2)):
        part = o_ref.at[:, pl.ds(h * wide, wide)]
        pltpu.make_async_copy(part, part, o_recv.at[h]).wait()

    for here, far, near in pieces + handed[0] + handed[1]:
        @pl.when(jnp.logical_not(here))
        def _(far=far):
            far.wait_send()

    @pl.when(is_source)
    def _():
        lam_copy().wait_send()

        @pl.loop(0, n)
        def _(w):
            s, r = source_of(w)
            for which in range(2):
                to_core(s, which).wait_send()

                @pl.when(r == 0)
                def _(which=which):
                    for k in range(1, group):
                        sideways(s, k, which).wait_send()


def attention(queries, key_rows, value_rows, lambdas, head_gain):
    n = lax.axis_size("sp")
    tp_size = lax.axis_size("tp")
    length, columns = queries.shape
    wide = 2 * DH
    heads = columns // wide
    group = n // (2 * heads)
    chunks = 4 * group
    size = length * n // chunks
    post = length // tp_size
    kind = jnp.bfloat16
    dma = pltpu.SemaphoreType.DMA
    vmem = pl.BlockSpec(memory_space=pltpu.VMEM)
    return pl.pallas_call(
        functools.partial(attention_kernel, n, group, heads, post),
        out_shape=jax.ShapeDtypeStruct((post, columns * tp_size), kind),
        in_specs=[vmem] * 5,
        out_specs=vmem,
        scratch_shapes=[
            pltpu.VMEM((n, length, wide), kind),
            pltpu.VMEM((n, wide, length), kind),
            pltpu.VMEM((heads, wide, length), kind),
            pltpu.VMEM((2, size, wide), kind),
            pltpu.VMEM((4, 2 * wide, size), kind),
            pltpu.VMEM((4, 8, size), jnp.float32),
            pltpu.VMEM((4, wide + 16, size), jnp.float32),
            pltpu.VMEM((2, size, wide), kind),
            pltpu.VMEM((8, wide), jnp.float32),
            dma((2 * heads,)),
            dma((n,)),
            dma((n,)),
            dma((n, group, 2)),
            dma((n, 2)),
            dma((heads * chunks // n,)),
            dma((2,)),
            dma((1,)),
            dma((1,)),
            dma((2 * (size // post),)),
            dma((heads * tp_size,)),
        ],
        compiler_params=pltpu.CompilerParams(
            collective_id=1, has_side_effects=True, vmem_limit_bytes=60000000
        ),
    )(
        queries,
        key_rows,
        value_rows,
        jnp.broadcast_to(lambdas[:, None, None], (heads, 8, wide)),
        head_gain[None, :],
    )


def local(
    queries,
    key_rows,
    value_rows,
    lambdas,
    head_gain,
    out_weight,
    stream,
    ffn_gain,
    routes,
    route_weight,
    gate_weight,
    up_weight,
    down_weight,
):
    heads_local = attention(queries, key_rows, value_rows, lambdas, head_gain)
    attended = stream.astype(jnp.float32) + jnp.dot(
        heads_local, out_weight, preferred_element_type=jnp.float32
    )
    normed = (
        attended
        * lax.rsqrt(jnp.mean(attended * attended, axis=-1, keepdims=True) + 1e-06)
        * ffn_gain
    ).astype(jnp.bfloat16)
    rows_local = normed.shape[0]
    width = normed.shape[1]
    top_count = routes.shape[1]
    sp_size = lax.axis_size("sp")
    experts = sp_size * gate_weight.shape[0]
    slots = max(2, (rows_local * top_count * 5 + 4 * experts - 1) // (4 * experts))
    slots = -(-slots // 16) * 16
    flat_routes = routes.reshape(-1)
    onehot = (flat_routes[:, None] == jnp.arange(experts, dtype=jnp.int32)[None, :]).astype(
        jnp.int32
    )
    before = jnp.cumsum(onehot, axis=0) - onehot
    slot = jnp.sum(before * onehot, axis=1)
    target = flat_routes * slots + slot
    placed = (target[:, None] == jnp.arange(experts * slots, dtype=jnp.int32)[None, :]).astype(
        jnp.float32
    )
    placed = placed.reshape(rows_local, top_count, experts * slots)
    dispatch = jnp.transpose(jnp.sum(placed, axis=1)).astype(jnp.bfloat16)
    combine = jnp.einsum("tk,tks->ts", route_weight, placed, precision=lax.Precision.HIGHEST)
    outgoing = (
        jnp.dot(dispatch, normed, preferred_element_type=jnp.float32)
        .astype(jnp.bfloat16)
        .reshape(experts, slots, width)
    )
    gate_local = gate_weight[0]
    up_local = up_weight[0]
    down_local = down_weight[0]
    returned = exchange_and_apply(outgoing, gate_local, up_local, down_local).reshape(
        experts * slots, width
    )
    routed = jnp.dot(combine, returned.astype(jnp.float32), precision=lax.Precision.HIGHEST)
    return (attended + routed).astype(jnp.bfloat16)


def solution(mesh):
    placed = (
        P("sp", "tp"),
        P("sp", "tp"),
        P("sp", "tp"),
        P("tp"),
        P(),
        P(),
        P(("sp", "tp"), None),
        P(),
        P(("sp", "tp"), None),
        P(("sp", "tp"), None),
        P("sp", None, "tp"),
        P("sp", None, "tp"),
        P("sp", "tp", None),
    )
    return jax.shard_map(
        local, mesh=mesh, in_specs=placed, out_specs=P(("sp", "tp"), None), check_vma=False
    )
```

```python
import functools
import math

import jax
import jax.numpy as jnp
from jax import lax
from jax.experimental import pallas as pl
from jax.experimental.pallas import tpu as pltpu
from jax.sharding import PartitionSpec as P

DH = 64


def moe_kernel(
    n,
    lanes,
    slots,
    out_ref,
    gate_hbm,
    up_hbm,
    down_hbm,
    stream_ref,
    spot_ref,
    share_ref,
    o_ref,
    back_ref,
    total_ref,
    share_cols,
    gate,
    up,
    down,
    rows,
    act,
    part,
    from_core,
    chip_sum,
    from_y,
    final,
    weight_sem,
    local_sem,
    a_send,
    a_recv,
    y_send,
    y_recv,
    c_send,
    c_recv,
    p_send,
    p_recv,
    q_send,
    q_recv,
    r_send,
    r_recv,
):
    sp = lax.axis_index("sp")
    tp = lax.axis_index("tp")
    core = tp % 2
    ypos = tp // 2
    other = ypos * 2 + (1 - core)
    half = lanes * slots

    def y_up(j):
        return ((ypos + j) % lanes) * 2 + core

    def y_down(j):
        return ((ypos + lanes - j) % lanes) * 2 + core

    def block(k, lane, j):
        return rows.at[k, pl.ds((lane * lanes + j) * slots, slots)]

    def remote(src, dst, send, recv, where):
        return pltpu.make_async_remote_copy(
            src_ref=src,
            dst_ref=dst,
            send_sem=send,
            recv_sem=recv,
            device_id=where,
            device_id_type=pl.DeviceIdType.MESH,
        )

    near = n // 2

    def order(i):
        return i

    def partner(k):
        goal = 0
        bit = 1
        while bit < n:
            goal = goal + (sp // bit + k // bit) % 2 * bit
            bit *= 2
        return goal

    def exchange(k):
        goal = partner(k)
        return remote(out_ref.at[goal], block(k, 0, 0), a_send.at[k], a_recv.at[k], (goal, tp))

    def across(k, j):
        return remote(
            block(k, 0, 0), block(k, 0, j), y_send.at[k, j], y_recv.at[k, j], (sp, y_up(j))
        )

    def relay(k, j):
        return remote(
            block(k, 0, j), block(k, 1, j), c_send.at[k, j], c_recv.at[k, j], (sp, other)
        )

    def core_part(i):
        k = order(i)
        return remote(
            part.at[i % 2, pl.ds(half, half)], from_core.at[k], p_send.at[k], p_recv.at[k], (sp, other)
        )

    def y_part(k, j):
        return remote(
            chip_sum.at[k, pl.ds(j * slots, slots)],
            from_y.at[k, pl.ds((j - 1) * slots, slots)],
            q_send.at[k, j],
            q_recv.at[k, j],
            (sp, y_down(j)),
        )

    def give_back(k):
        goal = partner(k)
        return remote(final.at[k], back_ref.at[sp], r_send.at[k], r_recv.at[k], (goal, tp))

    weights = [
        pltpu.make_async_copy(a, b, weight_sem.at[i])
        for i, (a, b) in enumerate(((gate_hbm, gate), (up_hbm, up), (down_hbm, down)))
    ]
    for copy in weights:
        copy.start()
    own = pltpu.make_async_copy(out_ref.at[sp], block(0, 0, 0), local_sem.at[0])
    own.start()

    barrier = pltpu.get_barrier_semaphore()
    for k in range(1, n):
        pl.semaphore_signal(
            barrier, inc=1, device_id=((sp + k) % n, tp), device_id_type=pl.DeviceIdType.MESH
        )
    for k in range(1, 2 * lanes):
        pl.semaphore_signal(
            barrier,
            inc=1,
            device_id=(sp, (tp + k) % (2 * lanes)),
            device_id_type=pl.DeviceIdType.MESH,
        )
    pl.semaphore_wait(barrier, n + 2 * lanes - 2)

    @pl.loop(1, n)
    def _(k):
        exchange(k).start()

    def forward(k):
        for j in range(1, lanes):
            across(k, j).start()
        relay(k, 0).start()

    own.wait()
    forward(0)
    total_ref[...] = stream_ref[...]

    tile = math.gcd(gate.shape[1], 256)
    wide = math.gcd(down.shape[1], 256)

    def enter(i):
        k = order(i)
        exchange(k).wait_recv()
        forward(k)

    def spread(i):
        k = order(i)
        for j in range(1, lanes):
            across(k, j).wait_recv()
            relay(k, j).start()

    def compute(i):
        k = order(i)

        @pl.when(i == 0)
        def _():
            for copy in weights:
                copy.wait()

        for j in range(lanes):
            relay(k, j).wait_recv()

        @pl.when(i >= 2)
        def _():
            core_part(i - 2).wait_send()

        @pl.loop(0, gate.shape[1] // tile)
        def _(f):
            cols = pl.ds(pl.multiple_of(f * tile, tile), tile)
            x = rows[k]
            g = jnp.dot(x, gate[:, cols], preferred_element_type=jnp.float32)
            u = jnp.dot(x, up[:, cols], preferred_element_type=jnp.float32)
            act[:, cols] = (g / (1.0 + jnp.exp(-g)) * u).astype(jnp.bfloat16)

        @pl.loop(0, down.shape[1] // wide)
        def _(d):
            cols = pl.ds(pl.multiple_of(d * wide, wide), wide)
            part[i % 2, :, cols] = jnp.dot(
                act[...], down[:, cols], preferred_element_type=jnp.float32
            ).astype(jnp.bfloat16)

        core_part(i).start()

    def reduce(i):
        k = order(i)
        core_part(i).wait_recv()

        @pl.loop(0, half // 16)
        def _(r):
            at = pl.ds(pl.multiple_of(r * 16, 16), 16)
            total = part[i % 2, at].astype(jnp.float32) + from_core[k, at].astype(jnp.float32)
            chip_sum[k, at] = total.astype(jnp.bfloat16)

    def cross(i):
        for j in range(1, lanes):
            y_part(order(i), j).start()

    def finish(i):
        k = order(i)
        for j in range(1, lanes):
            y_part(k, j).wait_recv()

        @pl.loop(0, slots // 16)
        def _(r):
            at = pl.ds(pl.multiple_of(r * 16, 16), 16)
            total = chip_sum[k, at].astype(jnp.float32)
            for j in range(1, lanes):
                here = pl.ds(pl.multiple_of((j - 1) * slots + r * 16, 16), 16)
                total = total + from_y[k, here].astype(jnp.float32)
            final[k, at] = total.astype(jnp.bfloat16)

        @pl.when(k > 0)
        def _():
            give_back(k).start()

        @pl.when(k == 0)
        def _():
            pltpu.make_async_copy(final.at[0], back_ref.at[sp], local_sem.at[1]).start()

    rows_here = spot_ref.shape[0]
    top_count = spot_ref.shape[1]
    shares = jnp.transpose(jnp.concatenate([share_ref[...]] * (8 // top_count), axis=0))
    share_cols[...] = jnp.concatenate([shares] * 16, axis=1)

    def gather(e):
        lane = e * slots + lax.broadcasted_iota(jnp.int32, (rows_here, slots), 1)
        hits = [
            (spot_ref[:, c : c + 1] == lane).astype(jnp.float32).astype(jnp.bfloat16)
            for c in range(spot_ref.shape[1])
        ]

        @pl.loop(0, down.shape[1] // wide)
        def _(d):
            cols = pl.ds(pl.multiple_of(d * wide, wide), wide)
            total = total_ref[:, cols]
            for c, hit in enumerate(hits):
                row = jnp.dot(hit, back_ref[e, :, cols], preferred_element_type=jnp.float32)
                total = total + share_cols[:, c : c + 1] * row
            total_ref[:, cols] = total

    def urgent(i):
        return (i == 0) | (i >= near)

    @pl.loop(0, n + 3)
    def _(i):
        @pl.when(i < n - 1)
        def _():
            enter(i + 1)

        @pl.when(i < n)
        def _():
            spread(i)

        @pl.when((i >= 1) & (i < n + 1))
        def _():
            compute(i - 1)

        @pl.when((i >= 2) & (i < n + 2))
        def _():
            reduce(i - 2)

            @pl.when(urgent(i - 2))
            def _():
                cross(i - 2)

        @pl.when(i == n + 1)
        def _():
            @pl.loop(1, near)
            def _(k):
                cross(k)

        @pl.when((i >= 3) & urgent(i - 3))
        def _():
            finish(i - 3)

    @pl.loop(1, near)
    def _(k):
        finish(k)

    pltpu.make_async_copy(final.at[0], back_ref.at[sp], local_sem.at[1]).wait()

    @pl.loop(0, n)
    def _(i):
        k = i // 2 + i % 2 * near

        @pl.when(k > 0)
        def _():
            give_back(k).wait_recv()

        gather(partner(k))

    @pl.loop(0, down.shape[1] // wide)
    def _(d):
        cols = pl.ds(pl.multiple_of(d * wide, wide), wide)
        o_ref[:, cols] = total_ref[:, cols].astype(jnp.bfloat16)

    for i in (n - 2, n - 1):
        core_part(i).wait_send()

    @pl.loop(0, n)
    def _(k):
        @pl.when(k > 0)
        def _():
            exchange(k).wait_send()
            give_back(k).wait_send()

        for j in range(1, lanes):
            across(k, j).wait_send()
            y_part(k, j).wait_send()
        for j in range(lanes):
            relay(k, j).wait_send()


def exchange_and_apply(outgoing, gate_local, up_local, down_local, attended, spots, shares):
    n, slots, width = outgoing.shape
    lanes = lax.axis_size("tp") // 2
    hidden = gate_local.shape[1]
    kind = jnp.bfloat16
    dma = pltpu.SemaphoreType.DMA
    flops = 6 * n * lanes * 2 * slots * width * hidden
    return pl.pallas_call(
        functools.partial(moe_kernel, n, lanes, slots),
        out_shape=jax.ShapeDtypeStruct(attended.shape, kind),
        in_specs=[pl.BlockSpec(memory_space=pltpu.VMEM)]
        + [pl.BlockSpec(memory_space=pl.ANY)] * 3
        + [pl.BlockSpec(memory_space=pltpu.VMEM)] * 3,
        out_specs=pl.BlockSpec(memory_space=pltpu.VMEM),
        scratch_shapes=[
            pltpu.VMEM((n, slots, width), kind),
            pltpu.VMEM(attended.shape, jnp.float32),
            pltpu.VMEM((attended.shape[0], 128), jnp.float32),
            pltpu.VMEM((width, hidden), kind),
            pltpu.VMEM((width, hidden), kind),
            pltpu.VMEM((hidden, width), kind),
            pltpu.VMEM((n, 2 * lanes * slots, width), kind),
            pltpu.VMEM((2 * lanes * slots, hidden), kind),
            pltpu.VMEM((2, 2 * lanes * slots, width), kind),
            pltpu.VMEM((n, lanes * slots, width), kind),
            pltpu.VMEM((n, lanes * slots, width), kind),
            pltpu.VMEM((n, max(1, lanes - 1) * slots, width), kind),
            pltpu.VMEM((n, slots, width), kind),
            dma((3,)),
            dma((2,)),
            dma((n,)),
            dma((n,)),
            dma((n, lanes)),
            dma((n, lanes)),
            dma((n, lanes)),
            dma((n, lanes)),
            dma((n,)),
            dma((n,)),
            dma((n, lanes)),
            dma((n, lanes)),
            dma((n,)),
            dma((n,)),
        ],
        compiler_params=pltpu.CompilerParams(
            collective_id=0, has_side_effects=True, vmem_limit_bytes=67000000
        ),
        cost_estimate=pl.CostEstimate(
            flops=flops, bytes_accessed=6 * width * hidden, transcendentals=0
        ),
    )(outgoing, gate_local, up_local, down_local, attended, spots, shares)


def attention_kernel(
    n,
    group,
    heads,
    post,
    q_ref,
    k_ref,
    v_ref,
    lam_ref,
    gain_ref,
    o_ref,
    keys,
    values,
    turned,
    asked,
    masked_q,
    maxima,
    accum,
    done,
    lam,
    lam_out,
    kv_send,
    k_recv,
    v_recv,
    side_send,
    core_send,
    q_send,
    q_recv,
    lam_send,
    lam_recv,
    o_send,
    o_recv,
):
    sp = lax.axis_index("sp")
    tp = lax.axis_index("tp")
    tp_size = lax.axis_size("tp")
    core = tp % 2
    plane = tp // 2
    other = plane * 2 + (1 - core)
    in_plane = 2 * heads
    head = sp // group
    seat = sp % group
    source_core = head // heads
    is_source = core == source_core
    length = q_ref.shape[0]
    wide = 2 * DH
    chunks = 4 * group
    per_block = chunks // n
    size = length // per_block
    place = seat * 2 + core
    chunk_of = (place, chunks - 1 - place)
    parts = size // post

    def remote(src, dst, send, recv, where):
        return pltpu.make_async_remote_copy(
            src_ref=src,
            dst_ref=dst,
            send_sem=send,
            recv_sem=recv,
            device_id=where,
            device_id_type=pl.DeviceIdType.MESH,
        )

    barrier = pltpu.get_barrier_semaphore()
    everyone = n * tp_size
    me = sp * tp_size + tp

    @pl.loop(1, everyone)
    def _(k):
        to = (me + k) % everyone
        pl.semaphore_signal(
            barrier,
            inc=1,
            device_id=(to // tp_size, to % tp_size),
            device_id_type=pl.DeviceIdType.MESH,
        )

    lam_out[...] = jnp.full(lam_out.shape, lam_ref[head % heads], jnp.float32)
    pl.semaphore_wait(barrier, everyone - 1)

    def columns(h):
        return pl.ds(pl.multiple_of(h * wide, wide), wide)

    def turn_of(k):
        return jnp.where(head % 2 == 1, heads - 1 - k, k)

    def q_piece(k, i):
        h = turn_of(k)
        chunk = sp * per_block + i
        late = chunk >= 2 * group
        spot = jnp.where(late, chunks - 1 - chunk, chunk)
        slot = jnp.where(late, 1, 0)
        goal = (core * heads + h) * group + spot // 2
        goal_core = spot % 2
        src = q_ref.at[pl.ds(i * size, size), columns(h)]
        here = (goal == sp) & (goal_core == core)
        sem = q_send.at[k * per_block + i]
        far = remote(
            src, asked.at[slot], sem, q_recv.at[slot], (goal, plane * 2 + goal_core)
        )
        near = pltpu.make_async_copy(src, asked.at[slot], q_recv.at[slot])
        return here, far, near

    def kv_piece(k, which):
        h = turn_of(k)
        goal_head = core * heads + h
        here = goal_head == head
        src = k_ref.at[:, columns(h)] if which == 0 else turned.at[h]
        dst = (keys if which == 0 else values).at[sp]
        recv = (k_recv if which == 0 else v_recv).at[sp]
        far = remote(
            src, dst, kv_send.at[k * 2 + which], recv, (goal_head * group + seat, tp)
        )
        near = pltpu.make_async_copy(src, dst, recv)
        return here, far, near

    def launch(here, far, near):
        @pl.when(here)
        def _():
            near.start()

        @pl.when(jnp.logical_not(here))
        def _():
            far.start()

    pieces = [q_piece(k, i) for k in range(heads) for i in range(per_block)]
    pieces.append(kv_piece(0, 0))
    for piece in pieces:
        launch(*piece)
    for h in range(heads):
        block = v_ref[:, h * wide : (h + 1) * wide].astype(jnp.float32)
        turned[h] = jnp.transpose(block).astype(jnp.bfloat16)
    later = [kv_piece(0, 1)] + [kv_piece(k, which) for k in range(1, heads) for which in range(2)]
    for piece in later:
        launch(*piece)
    pieces += later
    for row in range(4):
        accum[row] = jnp.zeros(accum.shape[1:], jnp.float32)
        maxima[row] = jnp.full(maxima.shape[1:], -1e30, jnp.float32)

    def lam_copy():
        return remote(
            lam_out, lam, lam_send.at[0], lam_recv.at[0], (sp, other)
        )

    @pl.when(is_source)
    def _():
        lam_copy().start()

    lane = lax.broadcasted_iota(jnp.int32, (wide, size), 0)
    for slot in range(2):
        pltpu.make_async_copy(asked.at[slot], asked.at[slot], q_recv.at[slot]).wait()
        turn = jnp.transpose(asked[slot].astype(jnp.float32)) * (DH ** (-0.5) * math.log2(math.e))
        high = turn.astype(jnp.bfloat16)
        low = (turn - high.astype(jnp.float32)).astype(jnp.bfloat16)
        for m in range(2):
            keep = (lane >= m * DH) & (lane < (m + 1) * DH)
            masked_q[slot * 2 + m, 0:wide] = jnp.where(keep, high, jnp.zeros_like(high))
            masked_q[slot * 2 + m, wide : 2 * wide] = jnp.where(keep, low, jnp.zeros_like(low))

    def source_of(w):
        t = w // group
        r = w % group
        b = (head % 2 + t % 2) % 2 + 2 * ((head // 2 + t // 2) % 2)
        return b * group + (seat + r) % group, r

    def sideways(s, r, which):
        buf = (keys if which == 0 else values).at[s]
        recv = (k_recv if which == 0 else v_recv).at[s]
        goal = head * group + (seat + r) % group
        return remote(buf, buf, side_send.at[s, r, which], recv, (goal, tp))

    def to_core(s, which):
        buf = (keys if which == 0 else values).at[s]
        recv = (k_recv if which == 0 else v_recv).at[s]
        return remote(buf, buf, core_send.at[s, which], recv, (sp, other))

    def receive(w):
        s, r = source_of(w)
        for which in range(2):
            to_core(s, which).wait_recv()

            @pl.when(is_source)
            def _(which=which):
                @pl.when(r == 0)
                def _():
                    for k in range(1, group):
                        sideways(s, k, which).start()

                to_core(s, which).start()

    tall = math.gcd(length, 512)

    def attend(slot, s, chunk, diagonal):
        for first in range(0, length, tall):
            k = keys[s, first : first + tall]
            k = jnp.concatenate([k, k], axis=1)
            v = values[s, :, first : first + tall]
            v = jnp.concatenate([v, jnp.ones((16, tall), jnp.bfloat16)], axis=0)
            for m in range(2):
                row = slot * 2 + m
                scores = jnp.dot(k, masked_q[row], preferred_element_type=jnp.float32)
                if diagonal:
                    k_pos = s * length + first + lax.broadcasted_iota(jnp.int32, scores.shape, 0)
                    q_pos = chunk * size + lax.broadcasted_iota(jnp.int32, scores.shape, 1)
                    scores = jnp.where(k_pos <= q_pos, scores, -1e30)
                old = maxima[row, 0:1]
                top = jnp.maximum(jnp.max(scores, axis=0, keepdims=True), old)
                weights = jnp.exp2(scores - top).astype(jnp.bfloat16)
                mixed = jnp.dot(v, weights, preferred_element_type=jnp.float32)
                accum[row] = accum[row] * jnp.exp2(old - top) + mixed
                maxima[row] = jnp.broadcast_to(top, maxima.shape[1:])

    def step(slot, w):
        s, _ = source_of(w)
        chunk = jnp.where(slot == 0, chunk_of[0], chunk_of[1])
        block = chunk // per_block

        @pl.when(s == block)
        def _():
            attend(slot, s, chunk, True)

        @pl.when(s < block)
        def _():
            attend(slot, s, chunk, False)

    def slot_of(i):
        return jnp.where(2 * sp < n, 1 - i, i)

    rounds = n // group

    receive(0)

    @pl.loop(0, rounds)
    def _(t):
        @pl.loop(0, group)
        def _(r):
            @pl.when(r > 0)
            def _():
                receive(t * group + r)

            @pl.when((r == group - 1) & (t < rounds - 1))
            def _():
                receive((t + 1) * group)

            @pl.loop(0, jnp.where(t < rounds - 1, 2, 1))
            def _(i):
                step(slot_of(i), t * group + r)

    @pl.when(is_source)
    def _():
        lam[...] = lam_out[...]

    @pl.when(jnp.logical_not(is_source))
    def _():
        lam_copy().wait_recv()

    full_head = plane * in_plane + head

    def hand_over(slot, i):
        chunk = chunk_of[slot]
        goal = chunk // per_block
        goal_tp = (chunk % per_block) * parts + i
        here = (goal == sp) & (goal_tp == tp)
        src = done.at[slot, pl.ds(i * post, post)]
        dst = o_ref.at[:, pl.ds(pl.multiple_of(full_head * wide, wide), wide)]
        far = remote(src, dst, o_send.at[slot * parts + i], o_recv.at[full_head], (goal, goal_tp))
        near = pltpu.make_async_copy(src, dst, o_recv.at[full_head])
        return here, far, near

    handed = [[hand_over(slot, i) for i in range(parts)] for slot in range(2)]

    @pl.loop(0, 2)
    def _(i):
        slot = slot_of(i)

        @pl.when(i == 1)
        def _():
            @pl.loop(n - group, n)
            def _(w):
                step(slot, w)

        one = accum[slot * 2, 0:wide] * (1.0 / accum[slot * 2, wide : wide + 1])
        two = accum[slot * 2 + 1, 0:wide] * (1.0 / accum[slot * 2 + 1, wide : wide + 1])
        contrast = one - lam[0:1, 0:1] * two
        square = jnp.mean(contrast * contrast, axis=0, keepdims=True)
        contrast = jnp.transpose(contrast * lax.rsqrt(square + 1e-05)) * gain_ref[...]
        done[slot] = contrast.astype(jnp.bfloat16)
        for k in range(2):
            @pl.when(slot == k)
            def _(k=k):
                for piece in handed[k]:
                    launch(*piece)

    for h in range(in_plane * (tp_size // 2)):
        part = o_ref.at[:, pl.ds(h * wide, wide)]
        pltpu.make_async_copy(part, part, o_recv.at[h]).wait()

    for here, far, near in pieces + handed[0] + handed[1]:
        @pl.when(jnp.logical_not(here))
        def _(far=far):
            far.wait_send()

    @pl.when(is_source)
    def _():
        lam_copy().wait_send()

        @pl.loop(0, n)
        def _(w):
            s, r = source_of(w)
            for which in range(2):
                to_core(s, which).wait_send()

                @pl.when(r == 0)
                def _(which=which):
                    for k in range(1, group):
                        sideways(s, k, which).wait_send()


def attention(queries, key_rows, value_rows, lambdas, head_gain):
    n = lax.axis_size("sp")
    tp_size = lax.axis_size("tp")
    length, columns = queries.shape
    wide = 2 * DH
    heads = columns // wide
    group = n // (2 * heads)
    chunks = 4 * group
    size = length * n // chunks
    post = length // tp_size
    kind = jnp.bfloat16
    dma = pltpu.SemaphoreType.DMA
    vmem = pl.BlockSpec(memory_space=pltpu.VMEM)
    return pl.pallas_call(
        functools.partial(attention_kernel, n, group, heads, post),
        out_shape=jax.ShapeDtypeStruct((post, columns * tp_size), kind),
        in_specs=[vmem] * 3 + [pl.BlockSpec(memory_space=pltpu.SMEM), vmem],
        out_specs=vmem,
        scratch_shapes=[
            pltpu.VMEM((n, length, wide), kind),
            pltpu.VMEM((n, wide, length), kind),
            pltpu.VMEM((heads, wide, length), kind),
            pltpu.VMEM((2, size, wide), kind),
            pltpu.VMEM((4, 2 * wide, size), kind),
            pltpu.VMEM((4, 8, size), jnp.float32),
            pltpu.VMEM((4, wide + 16, size), jnp.float32),
            pltpu.VMEM((2, size, wide), kind),
            pltpu.VMEM((8, wide), jnp.float32),
            pltpu.VMEM((8, wide), jnp.float32),
            dma((2 * heads,)),
            dma((n,)),
            dma((n,)),
            dma((n, group, 2)),
            dma((n, 2)),
            dma((heads * chunks // n,)),
            dma((2,)),
            dma((1,)),
            dma((1,)),
            dma((2 * (size // post),)),
            dma((heads * tp_size,)),
        ],
        compiler_params=pltpu.CompilerParams(
            collective_id=1, has_side_effects=True, vmem_limit_bytes=60000000
        ),
    )(
        queries,
        key_rows,
        value_rows,
        lambdas,
        head_gain[None, :],
    )


def local(
    queries,
    key_rows,
    value_rows,
    lambdas,
    head_gain,
    out_weight,
    stream,
    ffn_gain,
    routes,
    route_weight,
    gate_weight,
    up_weight,
    down_weight,
):
    heads_local = attention(queries, key_rows, value_rows, lambdas, head_gain)
    attended = stream.astype(jnp.float32) + jnp.dot(
        heads_local, out_weight, preferred_element_type=jnp.float32
    )
    normed = (
        attended
        * lax.rsqrt(jnp.mean(attended * attended, axis=-1, keepdims=True) + 1e-06)
        * ffn_gain
    ).astype(jnp.bfloat16)
    rows_local = normed.shape[0]
    width = normed.shape[1]
    top_count = routes.shape[1]
    sp_size = lax.axis_size("sp")
    experts = sp_size * gate_weight.shape[0]
    slots = max(2, (rows_local * top_count * 5 + 4 * experts - 1) // (4 * experts))
    slots = -(-slots // 16) * 16
    flat_routes = routes.reshape(-1)
    onehot = (flat_routes[:, None] == jnp.arange(experts, dtype=jnp.int32)[None, :]).astype(
        jnp.int32
    )
    before = jnp.cumsum(onehot, axis=0) - onehot
    slot = jnp.sum(before * onehot, axis=1)
    target = flat_routes * slots + slot
    placed = (target[:, None] == jnp.arange(experts * slots, dtype=jnp.int32)[None, :]).astype(
        jnp.float32
    )
    placed = placed.reshape(rows_local, top_count, experts * slots)
    dispatch = jnp.transpose(jnp.sum(placed, axis=1)).astype(jnp.bfloat16)
    outgoing = (
        jnp.dot(dispatch, normed, preferred_element_type=jnp.float32)
        .astype(jnp.bfloat16)
        .reshape(experts, slots, width)
    )
    gate_local = gate_weight[0]
    up_local = up_weight[0]
    down_local = down_weight[0]
    return exchange_and_apply(
        outgoing,
        gate_local,
        up_local,
        down_local,
        attended,
        target.reshape(rows_local, top_count),
        route_weight.T,
    )


def solution(mesh):
    placed = (
        P("sp", "tp"),
        P("sp", "tp"),
        P("sp", "tp"),
        P("tp"),
        P(),
        P(),
        P(("sp", "tp"), None),
        P(),
        P(("sp", "tp"), None),
        P(("sp", "tp"), None),
        P("sp", None, "tp"),
        P("sp", None, "tp"),
        P("sp", "tp", None),
    )
    return jax.shard_map(
        local, mesh=mesh, in_specs=placed, out_specs=P(("sp", "tp"), None), check_vma=False
    )
```
